32 devices in a mesh: ep: 16 (over z, y, x), tp: 2 (over core).
Axes of the slice: x: 2, y: 2, z: 4, core: 2. Of those that a mesh axis runs over, the one named last changes fastest.
Arguments:
- tokens: bfloat16 [2048, 2048], P('ep'), may hold values from -6 to 6
- expert_ids: int32 [2048, 2], P('ep'), may hold values from 0 to 7, all different within a row; in each aligned block of 128 rows (0 to 127, 128 to 255, ...) at most 64 rows name the same one
- route_weights: float32 [2048, 2], P('ep'), may hold values from 0.2 to 1
- norm_gain: float32 [2048], replicated, may hold values from 0.1 to 1.9
- gate_weight: bfloat16 [2048, 8192], P(None, ('ep', 'tp')), may hold values from -0.125 to 0.125
- up_weight: bfloat16 [2048, 8192], P(None, ('ep', 'tp')), may hold values from -0.125 to 0.125
- down_weight: bfloat16 [8192, 2048], P('ep', 'tp'), may hold values from -0.1875 to 0.1875
- dense_gate: bfloat16 [2048, 256], P('ep'), may hold values from -0.125 to 0.125
- dense_up: bfloat16 [2048, 256], P('ep'), may hold values from -0.125 to 0.125
- dense_down: bfloat16 [256, 2048], P(None, 'tp'), may hold values from -0.375 to 0.375
- branch_gate: float32 [2048], P('tp'), may hold values from -3 to 3
Outputs:
- mixed: bfloat16 [2048, 2048], P('ep', 'tp')
The draws below stay inside these ranges and needn't reach their ends.
Inputs may be any that keep to these rules, and one draw needn't show every extreme that they name: `expert_ids`: each row names 2 different experts. Within the rows of one device (aligned blocks of 128 rows) no expert is named more than 64 times; in some blocks an expert is named exactly 64 times.
All inputs are finite; a program needn't handle non-finite values.
Results may differ from the reference program's by a relative error of at most 0.0074.
Values may be sent and summed in bfloat16 or wider, within the bound.
No kernel may reach another device: no remote copies, remote signals or barrier semaphores. Data moves between devices by JAX's collectives and lax.ppermute only.
A program may use at most 64 MiB of HBM per device.

```python
import math
import jax
import jax.numpy as jnp
import numpy as np
from jax import lax

D = 2048
FF = 1024
SH = 256
TOP = 2
TOK_DEV = 128
EXPERTS = 8
TOKENS = 2048
SLOTS = 64
N_EP = 16


def levels(stream_key, dims, pieces, least, top_value):
    loudness, own = 1.0, jax.random.fold_in(stream_key, 6)
    for dim, blocks in pieces:
        heights = jnp.exp(jax.random.uniform(jax.random.fold_in(own, dim), (blocks,), jnp.float32, least / len(pieces), top_value / len(pieces)))
        loudness = loudness * jnp.repeat(heights, dims[dim] // blocks).reshape([-1 if axis == dim else 1 for axis in range(len(dims))])
    return loudness


def deal_out(key, own, number, rows, count, top, limit, skew):
    order = jax.random.permutation(key, count)
    crowded, common = portions_of(count, rows * top, limit, skew, True), portions_of(count, rows * top, limit, skew, False)
    places = jnp.arange(count)

    def named(tallies, rotation):
        used = int((tallies > 0).sum())
        fixed = max(1, used // 4)
        passed = fixed + (places - fixed + rotation * (used - fixed)) % max(1, count - fixed)
        return jnp.zeros((count,), jnp.int32).at[order[jnp.where(places < fixed, places, passed)]].set(jnp.asarray(tallies, jnp.int32))

    tallies = jnp.where(number % 4 == 0, named(crowded, number // 4), named(common, number - number // 4 - 1))
    mixed = jax.random.permutation(jax.random.fold_in(own, 3), count)
    source_of, taker = mixed[0:count // 2 * 2:2], mixed[1:count // 2 * 2:2]
    room = jnp.minimum(tallies[source_of] - 1, limit - tallies[taker]) // 2
    room = jnp.where((source_of == order[0]) | (taker == order[0]) | (tallies[taker] == 0), 0, jnp.maximum(room, 0))
    passed = jax.random.randint(jax.random.fold_in(own, 4), (count // 2,), 0, 1 << 20) % (room + 1)
    tallies = tallies.at[source_of].add(-passed).at[taker].add(passed)
    items = jnp.searchsorted(jnp.cumsum(tallies), jnp.arange(rows * top), side="right").astype(jnp.int32)
    table = items.reshape(top, rows).T
    table = table[jax.random.permutation(jax.random.fold_in(own, 1), rows)]
    rotation = jax.random.randint(jax.random.fold_in(own, 2), (rows, 1), 0, top)
    return jnp.take_along_axis(table, (jnp.arange(top)[None, :] + rotation) % top, axis=1)


def portions_of(number_of, total, bound, lean, full):
    weights = [(1 << 20) // math.isqrt(grade ** lean) + 1 for grade in range(1, number_of + 1)]
    largest = bound if full else min(bound, max(-(-total // number_of), total * weights[0] // sum(weights)))
    least = 1 if total - largest >= number_of - 1 else 0
    given, spare = [largest] + [least] * (number_of - 1), total - largest - least * (number_of - 1)
    while spare > 0:
        candidates = [i for i in range(1, number_of) if given[i] < largest] or [i for i in range(1, number_of) if given[i] < bound]
        pool, remaining = sum([weights[i] for i in candidates]), spare
        for i in candidates:
            extra = min(bound - given[i], max(1, remaining * weights[i] // pool), spare)
            given[i] = given[i] + extra
            spare = spare - extra
    return np.array(given)


def noise(own_key, shape, width, reach, pieces=(), kind=jnp.bfloat16):
    drawn = width * jax.random.normal(own_key, shape, jnp.float32)
    if pieces:
        drawn = drawn * levels(own_key, shape, pieces, -0.22, 0.18)
    return jnp.clip(drawn, -reach, reach).astype(kind)


def setup_inputs(seed: int = 0) -> dict:
    keys = jax.random.split(jax.random.key(seed), 12)
    tokens = noise(keys[0], (TOKENS, D), 1.0, 6.0, ((0, 16),))
    expert_ids_keys = jax.random.split(jax.random.fold_in(keys[1], 1), TOKENS // TOK_DEV)
    expert_ids_turns = jax.random.permutation(jax.random.fold_in(keys[1], 3), TOKENS // TOK_DEV)
    expert_ids = jax.vmap(lambda own, number: deal_out(jax.random.fold_in(keys[1], 2), own, number, TOK_DEV, EXPERTS, TOP, SLOTS, 2))(expert_ids_keys, expert_ids_turns).reshape((TOKENS, TOP))
    route_weights = jnp.clip(0.2 + 0.8 * jax.random.uniform(keys[2], (TOKENS, TOP), jnp.float32) ** levels(keys[2], (TOKENS, TOP), ((0, 16),), -0.2, 0.2), 0.2, 1.0)
    norm_gain = jnp.clip(1.0 + 0.18 * jax.random.normal(keys[3], (D,), jnp.float32), 0.1, 1.9)
    gate_weight = noise(keys[4], (D, EXPERTS * FF), D ** -0.5, 0.125, ((1, 32),))
    up_weight = noise(keys[5], (D, EXPERTS * FF), D ** -0.5, 0.125, ((1, 32),))
    down_weight = noise(keys[6], (EXPERTS * FF, D), FF ** -0.5, 0.1875, ((0, 16), (1, 2)))
    dense_gate = noise(keys[7], (D, SH), D ** -0.5, 0.125, ((0, 16),))
    dense_up = noise(keys[8], (D, SH), D ** -0.5, 0.125, ((0, 16),))
    dense_down = noise(keys[9], (SH, D), SH ** -0.5, 0.375, ((1, 2),))
    branch_gate = jnp.clip(jax.random.uniform(keys[10], (D,), jnp.float32, -3.0, 3.0) * levels(keys[10], (D,), ((0, 2),), -0.4, 0.0), -3.0, 3.0)
    return dict(tokens=tokens, expert_ids=expert_ids, route_weights=route_weights, norm_gain=norm_gain, gate_weight=gate_weight, up_weight=up_weight, down_weight=down_weight, dense_gate=dense_gate, dense_up=dense_up, dense_down=dense_down, branch_gate=branch_gate)


epsilon = 1e-06

def reference(tokens, expert_ids, route_weights, norm_gain, gate_weight, up_weight, down_weight, dense_gate, dense_up, dense_down, branch_gate):
    model_width = tokens.shape[1]
    values = tokens.astype(jnp.float32)
    inverse = lax.rsqrt(lax.optimization_barrier(jnp.mean(values * values, axis=1, keepdims=True)) + epsilon)
    normed = (values * inverse * norm_gain[None, :]).astype(jnp.bfloat16)
    dense_gate_act = jnp.dot(normed, dense_gate, preferred_element_type=jnp.float32)
    dense_up_act = jnp.dot(normed, dense_up, preferred_element_type=jnp.float32)
    dense_hidden = (jax.nn.silu(dense_gate_act) * dense_up_act).astype(jnp.bfloat16)
    dense_out = jnp.dot(dense_hidden, dense_down, preferred_element_type=jnp.float32)
    flat_ids = expert_ids.reshape(N_EP, TOK_DEV * TOP)
    labels = jnp.arange(EXPERTS, dtype=jnp.int32)
    onehot = (flat_ids[:, :, None] == labels[None, None, :]).astype(jnp.int32)
    earlier = jnp.cumsum(onehot, axis=1) - onehot
    slot_index = lax.optimization_barrier(jnp.sum(onehot * earlier, axis=2)).astype(jnp.int32)
    source = jnp.arange(N_EP, dtype=jnp.int32)[:, None]
    slot_row = (source * SLOTS + slot_index).astype(jnp.int32)
    owner_rows = (jnp.arange(TOK_DEV * TOP, dtype=jnp.int32)[None, :] // TOP + source * TOK_DEV).astype(jnp.int32)
    row_table = jnp.full((EXPERTS, N_EP * SLOTS), TOKENS, jnp.int32)
    row_table = row_table.at[flat_ids.reshape(-1), slot_row.reshape(-1)].set(owner_rows.reshape(-1))
    padded = jnp.concatenate([normed, jnp.zeros((1, model_width), jnp.bfloat16)], axis=0)
    half_width = FF // 2

    def run_expert(expert_index):
        in_rows = padded[row_table[expert_index]]
        offset = (expert_index * FF).astype(jnp.int32)
        w_gate = lax.dynamic_slice_in_dim(gate_weight, offset, FF, 1)
        w_up = lax.dynamic_slice_in_dim(up_weight, offset, FF, 1)
        w_down = lax.dynamic_slice_in_dim(down_weight, offset, FF, 0)
        expert_gate = jnp.dot(in_rows, w_gate, preferred_element_type=jnp.float32)
        expert_up = jnp.dot(in_rows, w_up, preferred_element_type=jnp.float32)
        hidden = (jax.nn.silu(expert_gate) * expert_up).astype(jnp.bfloat16)
        lower_part = jnp.dot(hidden[:, :half_width], w_down[:half_width], preferred_element_type=jnp.float32).astype(jnp.bfloat16)
        upper_part = jnp.dot(hidden[:, half_width:], w_down[half_width:], preferred_element_type=jnp.float32).astype(jnp.bfloat16)
        return (lower_part.astype(jnp.float32) + upper_part.astype(jnp.float32)).astype(jnp.bfloat16)
    results = lax.map(run_expert, jnp.arange(EXPERTS, dtype=jnp.int32))
    picked = results[flat_ids.reshape(TOKENS, TOP), slot_row.reshape(TOKENS, TOP)]
    routed = lax.optimization_barrier(jnp.sum(route_weights[:, :, None] * picked.astype(jnp.float32), axis=1))
    mixed_out = routed + jax.nn.sigmoid(branch_gate)[None, :] * dense_out
    return mixed_out.astype(jnp.bfloat16)
```

```python
import functools

import jax
import jax.numpy as jnp
from jax import lax
from jax.experimental import pallas as pl
from jax.experimental.pallas import tpu as pltpu
from jax.sharding import PartitionSpec as P

epsilon = 1e-06
bf16 = jnp.bfloat16
f32 = jnp.float32


def swap_ep(value, mask):
    count = lax.axis_size("ep")
    return lax.ppermute(value, "ep", [(i, i ^ mask) for i in range(count)])


def swap_tp(value):
    count = lax.axis_size("tp")
    return lax.ppermute(value, "tp", [(i, count - 1 - i) for i in range(count)])


def dense_hidden_kernel(orders, ep_ref, normed_ref, *refs):
    piece_refs, out_ref = refs[:-1], refs[-1]
    block = piece_refs[0].shape[1]
    half = out_ref.shape[1]
    ep = ep_ref[0]
    total = None
    for piece_ref, rels in zip(piece_refs, orders):
        for i, rel in enumerate(rels):
            start = pl.multiple_of((ep ^ rel) * block, block)
            part = jnp.dot(
                normed_ref[:, pl.ds(start, block)], piece_ref[i], preferred_element_type=f32
            )
            total = part if total is None else total + part
    gate, up = total[:, :half], total[:, half:]
    out_ref[...] = (gate / (1.0 + jnp.exp(-gate)) * up).astype(bf16)


def dense_hidden_of(normed, dense_gate, dense_up):
    ep_count, tp_count = lax.axis_size("ep"), lax.axis_size("tp")
    columns = dense_gate.shape[1] // tp_count
    start = lax.axis_index("tp") * columns
    shard = jnp.concatenate(
        [
            lax.dynamic_slice_in_dim(dense_gate, start, columns, 1),
            lax.dynamic_slice_in_dim(dense_up, start, columns, 1),
        ],
        axis=1,
    )[None]
    bits = [1 << b for b in range(ep_count.bit_length() - 1)]
    bits = bits[2:] + bits[1:2] + bits[:1]
    pieces, orders, rels = [shard], [[0]], [0]
    for bit in bits:
        so_far = pieces[0] if len(pieces) == 1 else jnp.concatenate(pieces, axis=0)
        pieces.append(swap_ep(so_far, bit))
        orders.append([r ^ bit for r in rels])
        rels = rels + orders[-1]
    return pl.pallas_call(
        functools.partial(dense_hidden_kernel, orders),
        out_shape=jax.ShapeDtypeStruct((normed.shape[0], columns), bf16),
        in_specs=[pl.BlockSpec(memory_space=pltpu.SMEM)]
        + [pl.BlockSpec(memory_space=pltpu.VMEM)] * (1 + len(pieces)),
        out_specs=pl.BlockSpec(memory_space=pltpu.VMEM),
        name="dense_hidden",
    )(lax.axis_index("ep").reshape(1).astype(jnp.int32), normed, *pieces)


def by_planes(
    tokens,
    expert_ids,
    route_weights,
    norm_gain,
    gate_weight,
    up_weight,
    down_weight,
    dense_gate,
    dense_up,
    dense_down,
    branch_gate,
):
    tok_rows, model_width = tokens.shape
    ep_count = lax.axis_size("ep")
    experts = ep_count // 2
    slots = 2 * expert_ids.shape[1] * tok_rows // experts
    planes = ep_count // 4
    ep, tp = lax.axis_index("ep"), lax.axis_index("tp")
    half = model_width // 2
    my_expert = (ep // 2).astype(f32)
    other_expert = ((ep // 2) ^ 1).astype(f32)

    def own_rows(array):
        count = array.shape[0] // 2
        return (
            lax.dynamic_slice_in_dim(array, tp * count, count, 0),
            lax.dynamic_slice_in_dim(array, (1 - tp) * count, count, 0),
        )

    meta = jnp.concatenate([expert_ids.T.astype(f32), route_weights.T], axis=0)[None]
    for bit in range(planes.bit_length() - 1):
        meta = jnp.concatenate([meta, swap_ep(meta, 4 << bit)], axis=0)

    values = tokens.astype(f32)
    inverse = lax.rsqrt(jnp.mean(values * values, axis=1, keepdims=True) + epsilon)
    normed = (values * inverse * norm_gain[None, :]).astype(bf16)
    mine = lax.dynamic_slice_in_dim(normed, tp * half, half, 1)
    order = [1] + list(range(planes - 1, 1, -1)) if planes > 1 else []
    dense_rows = {0: mine}
    for c in order:
        dense_rows[c] = swap_ep(mine, 4 * c)

    top = expert_ids.shape[1]
    ids, weights = meta[:, :top], meta[:, top:]
    wanted = jnp.stack([my_expert, other_expert])
    match = ids[:, None] == wanted[None, :, None, None]
    named = jnp.any(match, axis=2)
    weight = jnp.sum(jnp.where(match, weights[:, None], 0.0), axis=2)
    before = (
        lax.broadcasted_iota(jnp.int32, (tok_rows, tok_rows), 0)
        < lax.broadcasted_iota(jnp.int32, (tok_rows, tok_rows), 1)
    ).astype(bf16)
    place = jnp.dot(
        named.astype(bf16).reshape(planes * 2, tok_rows), before, preferred_element_type=f32
    ).reshape(planes, 2, 1, tok_rows)
    slot = lax.broadcasted_iota(jnp.int32, (1, 1, slots, 1), 2).astype(f32)
    chosen = (place == slot) & named[:, :, None, :]
    selector = chosen.astype(bf16)
    spread = jnp.where(chosen, weight[:, :, None, :], 0.0)
    spread_high = spread.astype(bf16)
    spread_low = (spread - spread_high.astype(f32)).astype(bf16)

    gate_mine, gate_other = own_rows(gate_weight)
    up_mine, up_other = own_rows(up_weight)
    down_mine, down_other = own_rows(down_weight)

    def dot(a, b):
        return jnp.dot(a, b, preferred_element_type=f32)

    results = {}
    groups = [[0]] + [[c] for c in order]
    for group in groups:
        picked = [
            dot(selector[c].reshape(2 * slots, tok_rows), dense_rows[c]).astype(bf16) for c in group
        ]
        keep = jnp.concatenate([p[:slots] for p in picked], axis=0)
        pass_on = jnp.concatenate([p[slots:] for p in picked], axis=0)
        rows = jnp.concatenate(
            [keep, swap_ep(keep, 1), swap_ep(pass_on, 2), swap_ep(pass_on, 3)], axis=0
        )
        rows_other = swap_tp(rows)
        gate = dot(rows, gate_mine) + dot(rows_other, gate_other)
        up = dot(rows, up_mine) + dot(rows_other, up_other)
        hidden = (gate / (1.0 + jnp.exp(-gate)) * up).astype(bf16)
        hidden_other = swap_tp(hidden)
        part = (dot(hidden, down_mine) + dot(hidden_other, down_other)).astype(bf16)
        part = part.reshape(4, len(group), slots, half)
        back = [part[0], swap_ep(part[1], 1), swap_ep(part[2], 2), swap_ep(part[3], 3)]
        for i, c in enumerate(group):
            kept = (back[0][i].astype(f32) + back[1][i].astype(f32)).astype(bf16)
            passed = (back[2][i].astype(f32) + back[3][i].astype(f32)).astype(bf16)
            both = jnp.concatenate([kept, passed], axis=0)
            high = spread_high[c].reshape(2 * slots, tok_rows)
            low = spread_low[c].reshape(2 * slots, tok_rows)
            contract = (((0,), (0,)), ((), ()))
            mixed = lax.dot_general(
                high, both, contract, preferred_element_type=f32
            ) + lax.dot_general(low, both, contract, preferred_element_type=f32)
            results[c] = mixed if c == 0 else swap_ep(mixed.astype(bf16), 4 * c)

    dense_hidden = dense_hidden_of(normed, dense_gate, dense_up)
    dense_mine, dense_other = own_rows(dense_down)
    dense_out = dot(dense_hidden, dense_mine) + dot(swap_tp(dense_hidden), dense_other)
    total = results[0]
    for c in order:
        total = total + results[c].astype(f32)
    return (total + jax.nn.sigmoid(branch_gate)[None, :] * dense_out).astype(bf16)


def by_all_to_all(
    tokens,
    expert_ids,
    route_weights,
    norm_gain,
    gate_weight,
    up_weight,
    down_weight,
    dense_gate,
    dense_up,
    dense_down,
    branch_gate,
):
    tok_rows, model_width = tokens.shape
    top_count = expert_ids.shape[1]
    ep_count = lax.axis_size("ep")
    experts = ep_count // 2
    slot_count = 2 * top_count * tok_rows // experts
    values = tokens.astype(jnp.float32)
    inverse = lax.rsqrt(jnp.mean(values * values, axis=1, keepdims=True) + epsilon)
    normed = (values * inverse * norm_gain[None, :]).astype(jnp.bfloat16)
    dense_gate_act = jnp.dot(
        normed,
        lax.all_gather(dense_gate, "ep", axis=0, tiled=True),
        preferred_element_type=jnp.float32,
    )
    dense_up_act = jnp.dot(
        normed,
        lax.all_gather(dense_up, "ep", axis=0, tiled=True),
        preferred_element_type=jnp.float32,
    )
    dense_hidden = (jax.nn.silu(dense_gate_act) * dense_up_act).astype(jnp.bfloat16)
    dense_out = jnp.dot(dense_hidden, dense_down, preferred_element_type=jnp.float32)
    flat_ids = expert_ids.reshape(tok_rows * top_count)
    labels = lax.broadcasted_iota(jnp.int32, (1, experts), 1)
    onehot = (flat_ids[:, None] == labels).astype(jnp.int32)
    earlier = jnp.cumsum(onehot, axis=0) - onehot
    slot_index = jnp.sum(onehot * earlier, axis=1)
    row_code = (flat_ids * slot_count + slot_index).reshape(tok_rows, top_count)
    targets = lax.broadcasted_iota(jnp.int32, (experts * slot_count, 1, 1), 0)
    selector = jnp.any(row_code[None, :, :] == targets, axis=2).astype(jnp.bfloat16)
    buffer = jnp.dot(selector, normed, preferred_element_type=jnp.float32).astype(jnp.bfloat16)
    buffer = buffer.reshape(experts, slot_count, model_width)
    half = model_width // 2
    outgoing = lax.dynamic_slice_in_dim(
        jnp.repeat(buffer, 2, axis=0), lax.axis_index("tp") * half, half, 2
    )
    arrived = lax.all_gather(
        lax.all_to_all(outgoing, "ep", split_axis=0, concat_axis=0, tiled=True),
        "tp",
        axis=2,
        tiled=True,
    )
    in_rows = arrived.reshape(ep_count * slot_count, model_width)
    expert_gate = jnp.dot(in_rows, gate_weight, preferred_element_type=jnp.float32)
    expert_up = jnp.dot(in_rows, up_weight, preferred_element_type=jnp.float32)
    hidden = (jax.nn.silu(expert_gate) * expert_up).astype(jnp.bfloat16)
    down_total = jnp.dot(
        lax.all_gather(hidden, "tp", axis=1, tiled=True),
        down_weight,
        preferred_element_type=jnp.float32,
    )
    partial_value = down_total.astype(jnp.bfloat16).reshape(ep_count, slot_count, -1)
    returned_rows = lax.all_to_all(partial_value, "ep", split_axis=0, concat_axis=0, tiled=True)
    pair_sums = returned_rows.reshape(experts, 2, slot_count, -1).astype(jnp.float32)
    expert_out = (
        (pair_sums[:, 0] + pair_sums[:, 1]).astype(jnp.bfloat16).reshape(experts * slot_count, -1)
    )
    picked = (
        jnp.take(expert_out, row_code.reshape(-1), axis=0)
        .reshape(tok_rows, top_count, -1)
        .astype(jnp.float32)
    )
    routed = jnp.sum(route_weights[:, :, None] * picked, axis=1)
    mixed_out = routed + jax.nn.sigmoid(branch_gate)[None, :] * dense_out
    return mixed_out.astype(jnp.bfloat16)


def per_device(*args):
    tokens, expert_ids = args[:2]
    experts = lax.axis_size("ep") // 2
    slots = 2 * expert_ids.shape[1] * tokens.shape[0] // experts
    if 2 * slots >= tokens.shape[0]:
        return by_planes(*args)
    return by_all_to_all(*args)


def solution(mesh):
    in_specs = (
        P("ep", None),
        P("ep", None),
        P("ep", None),
        P(),
        P(None, ("ep", "tp")),
        P(None, ("ep", "tp")),
        P("ep", "tp"),
        P("ep", None),
        P("ep", None),
        P(None, "tp"),
        P("tp"),
    )
    return jax.shard_map(
        per_device, mesh=mesh, in_specs=in_specs, out_specs=P("ep", "tp"), check_vma=False
    )
```

```python
import functools

import jax
import jax.numpy as jnp
from jax import lax
from jax.experimental import pallas as pl
from jax.experimental.pallas import tpu as pltpu
from jax.sharding import PartitionSpec as P

epsilon = 1e-06
bf16 = jnp.bfloat16
f32 = jnp.float32
META_ROWS = 8


def swap_ep(value, mask):
    count = lax.axis_size("ep")
    return lax.ppermute(value, "ep", [(i, i ^ mask) for i in range(count)])


def swap_active(value, mask, per_half):
    count = lax.axis_size("ep")
    pairs = []
    for i in range(count):
        core = i // per_half
        pairs.append((2 * i + core, 2 * (i ^ mask) + core))
    return lax.ppermute(value, ("ep", "tp"), pairs)


def swap_tp(value):
    count = lax.axis_size("tp")
    return lax.ppermute(value, "tp", [(i, count - 1 - i) for i in range(count)])


def dot(a, b):
    return jnp.dot(a, b, preferred_element_type=f32)


def gated(gate, up):
    return (gate / (1.0 + jnp.exp(-gate)) * up).astype(bf16)


def call(kernel, outs, arrays, flops, scratch=()):
    moved = sum(a.size * a.dtype.itemsize for a in arrays)
    return pl.pallas_call(
        kernel,
        out_shape=outs,
        in_specs=[pl.BlockSpec(memory_space=pltpu.VMEM)] * len(arrays),
        out_specs=jax.tree.map(lambda _: pl.BlockSpec(memory_space=pltpu.VMEM), outs),
        cost_estimate=pl.CostEstimate(flops=flops, bytes_accessed=moved, transcendentals=0),
        compiler_params=pltpu.CompilerParams(vmem_limit_bytes=4 << 20),
        scratch_shapes=scratch,
    )(*[pltpu.with_memory_space_constraint(a, pltpu.VMEM) for a in arrays])


def shape(rows, columns, dtype=bf16):
    return pltpu.VMEM((rows, columns), dtype)


def both_halves(count):
    tp = lax.axis_index("tp")
    return [pl.ds(pl.multiple_of(i * count, count), count) for i in (tp, 1 - tp)]


def prepare_kernel(
    tokens_at,
    gain_at,
    ids_at,
    weights_at,
    gate_at,
    up_at,
    payload_ref,
    shard_ref,
    tokens_ref,
    gain_ref,
    ids_ref,
    weights_ref,
    normed_ref,
    sems,
):
    rows, width = tokens_ref.shape
    half = width // 2
    columns = shard_ref.shape[1] // 2
    mine = both_halves(columns)[0]
    copies = []
    for source, target in (
        (tokens_at, tokens_ref),
        (gain_at, gain_ref),
        (ids_at, ids_ref),
        (weights_at, weights_ref),
        (gate_at.at[:, mine], shard_ref.at[:, :columns]),
        (up_at.at[:, mine], shard_ref.at[:, columns:]),
    ):
        copies.append(pltpu.make_async_copy(source, target, sems.at[len(copies)]))
        copies[-1].start()
    for copy in copies[:4]:
        copy.wait()
    values = tokens_ref[...].astype(f32)
    inverse = lax.rsqrt(jnp.mean(values * values, axis=1, keepdims=True) + epsilon)
    normed_ref[...] = (values * inverse * gain_ref[...]).astype(bf16)
    payload_ref[:rows, :] = normed_ref[:, both_halves(half)[0]]
    payload_ref[rows:, :] = jnp.zeros((META_ROWS, half), bf16)
    weights = weights_ref[...]
    parts = [ids_ref[...].astype(f32)]
    for _ in range(3):
        parts.append(weights.astype(bf16).astype(f32))
        weights = weights - parts[-1]
    payload_ref[rows:, :rows] = jnp.concatenate(parts, axis=0).astype(bf16)
    for copy in copies[4:]:
        copy.wait()


def select_kernel(top, slots, payload_ref, *refs):
    rider_refs, (keep_ref, pass_ref, spread_ref) = refs[:-3], refs[-3:]
    tokens = payload_ref.shape[0] - META_ROWS
    before = (
        lax.broadcasted_iota(jnp.int32, (tokens, tokens), 0)
        < lax.broadcasted_iota(jnp.int32, (tokens, tokens), 1)
    ).astype(bf16)
    slot = lax.broadcasted_iota(jnp.int32, (slots, tokens), 0).astype(f32)
    meta = payload_ref[tokens:, :tokens].astype(f32)
    ids = meta[:top]
    weights = sum(meta[top * p : top * (p + 1)] for p in range(1, 4))
    for side, out_ref in enumerate((keep_ref, pass_ref)):
        match = ids == ((lax.axis_index("ep") // 2) ^ side).astype(f32)
        named = jnp.max(match.astype(f32), axis=0, keepdims=True)
        weight = jnp.sum(jnp.where(match, weights, 0.0), axis=0, keepdims=True)
        place = dot(jnp.broadcast_to(named, (META_ROWS, tokens)).astype(bf16), before)[:1]
        chosen = (place == slot) & (named > 0.0)
        out_ref[:slots, :] = dot(chosen.astype(bf16), payload_ref[:tokens, :]).astype(bf16)
        spread = jnp.where(chosen, weight, 0.0)
        high = spread.astype(bf16)
        low = (spread - high.astype(f32)).astype(bf16)
        here = slice(side * slots, (side + 1) * slots)
        spread_ref[here, :tokens] = high
        spread_ref[here, tokens:] = low
        for rider_ref in rider_refs:
            count, width = out_ref.shape[0] - slots, rider_ref.shape[1]
            for q in range(out_ref.shape[1] // width):
                out_ref[slots:, q * width : (q + 1) * width] = rider_ref[
                    q * count : (q + 1) * count, :
                ]


def hidden_kernel(spans, mine_ref, other_ref, gate_ref, up_ref, out_ref):
    mine, other = both_halves(mine_ref.shape[1])
    rows, rows_other = mine_ref[...], other_ref[...]
    gate = dot(rows, gate_ref[mine, :]) + dot(rows_other, gate_ref[other, :])
    up = dot(rows, up_ref[mine, :]) + dot(rows_other, up_ref[other, :])
    hidden = gated(gate, up)
    at = 0
    for start, count in spans:
        out_ref[at : at + count, :] = hidden[start : start + count]
        at += count


def down_kernel(rows, mine_ref, other_ref, down_ref, *out_refs):
    count = mine_ref.shape[1]
    mine, other = both_halves(count)
    total = dot(mine_ref[...], down_ref[mine, :]) + dot(other_ref[...], down_ref[other, :])
    for i, out_ref in enumerate(out_refs):
        out_ref[...] = total[i * rows : (i + 1) * rows].astype(bf16)


def combine_kernel(kept0_ref, kept1_ref, passed0_ref, passed1_ref, spread_ref, *refs):
    out_ref = refs[-1]
    tokens = out_ref.shape[0]
    slots = kept0_ref.shape[0]
    contract = (((0,), (0,)), ((), ()))
    total = None
    for side, (a_ref, b_ref) in enumerate(((kept0_ref, kept1_ref), (passed0_ref, passed1_ref))):
        both = (a_ref[...].astype(f32) + b_ref[...].astype(f32)).astype(bf16)
        at = side * slots
        for part in (slice(0, tokens), slice(tokens, 2 * tokens)):
            term = lax.dot_general(
                spread_ref[at : at + slots, part], both, contract, preferred_element_type=f32
            )
            total = term if total is None else total + term
    for ref in refs[:-1]:
        total = total + ref[...].astype(f32)
    out_ref[...] = total.astype(out_ref.dtype)


def dense_part_kernel(planes, rider_at, rider_rows, rows_ref, other_ref, *refs):
    payload_refs, out_refs, weights_ref = refs[:planes], refs[planes:-1], refs[-1]
    tokens = payload_refs[0].shape[0] - META_ROWS
    block = weights_ref.shape[0] // 4
    width = weights_ref.shape[1] // 2
    ep = lax.axis_index("ep")
    for i in range(4):
        first = rider_at[i]
        for side, source_ref in enumerate((rows_ref, other_ref)):
            for q in range(block // rider_rows):
                at = pl.multiple_of(((ep ^ i) % 4) * block + q * rider_rows, rider_rows)
                weights_ref[pl.ds(at, rider_rows), side * width : (side + 1) * width] = source_ref[
                    first : first + rider_rows, q * width : (q + 1) * width
                ]
    half_planes = planes // 2
    active = (ep // 4 // half_planes == lax.axis_index("tp")).astype(f32)
    start = pl.multiple_of((ep // 4) % half_planes * 4 * block, 4 * block)
    for n, payload_ref in enumerate(payload_refs):
        part = dot(payload_ref[:tokens, pl.ds(start, 4 * block)], weights_ref[...])
        part = (part * active).astype(bf16)
        out_refs[n % 2][n // 2] = part


def add_kernel(a_ref, b_ref, *out_refs):
    for n in range(a_ref.shape[0]):
        out_ref = out_refs[n % len(out_refs)]
        total = a_ref[n].astype(f32) + b_ref[n].astype(f32)
        out_ref[n // len(out_refs)] = total.astype(out_ref.dtype)


def finish_kernel(mine_ref, other_ref, down_ref, branch_ref, *refs):
    mine, other = mine_ref[0], other_ref[0]
    width = mine.shape[1] // 2
    count = width // 2
    dense = None
    for at, sums in zip(
        both_halves(count), (mine[:, :width] + other[:, width:], mine[:, width:] + other[:, :width])
    ):
        term = dot(gated(sums[:, :count], sums[:, count:]), down_ref[at, :])
        dense = term if dense is None else dense + term
    total = refs[0][...].astype(f32)
    for ref in refs[1:-1]:
        total = total + ref[...].astype(f32)
    refs[-1][...] = (total + jax.nn.sigmoid(branch_ref[...]) * dense).astype(bf16)


def by_planes(
    tokens,
    expert_ids,
    route_weights,
    norm_gain,
    gate_weight,
    up_weight,
    down_weight,
    dense_gate,
    dense_up,
    dense_down,
    branch_gate,
):
    tok_rows, model_width = tokens.shape
    top = expert_ids.shape[1]
    ep_count = lax.axis_size("ep")
    experts = ep_count // 2
    slots = 2 * top * tok_rows // experts
    planes = ep_count // 4
    half = model_width // 2

    columns = dense_gate.shape[1] // 2
    rows = dense_gate.shape[0]
    inputs = [tokens, norm_gain[None, :], expert_ids.T, route_weights.T, dense_gate, dense_up]
    payload, shard = pl.pallas_call(
        prepare_kernel,
        out_shape=(shape(tok_rows + META_ROWS, half), shape(rows, 2 * columns)),
        in_specs=[pl.BlockSpec(memory_space=pltpu.HBM)] * len(inputs),
        out_specs=[pl.BlockSpec(memory_space=pltpu.VMEM)] * 2,
        scratch_shapes=[pltpu.VMEM(a.shape, a.dtype) for a in inputs[:4]]
        + [pltpu.VMEM(tokens.shape, bf16), pltpu.SemaphoreType.DMA((len(inputs),))],
        compiler_params=pltpu.CompilerParams(vmem_limit_bytes=4 << 20),
        name="prepare",
    )(*[pltpu.with_memory_space_constraint(a, pltpu.HBM) for a in inputs])
    payloads = {0: payload}
    for c in range(1, planes):
        low = c & -c
        payloads[c] = swap_ep(payloads[c ^ low], 4 * low)

    rider_rows = shard.size // half

    results, relayed, dense_parts = [], {}, None
    for group in chunk_groups(planes):
        n = len(group)
        sent, spreads, spans, rider_at, at = [], {}, [], [], 0
        for c in group:
            riders = [] if c else [shard]
            size = slots + len(riders) * rider_rows
            keep, pass_on, spreads[c] = call(
                functools.partial(select_kernel, top, slots),
                (shape(size, half), shape(size, half), shape(2 * slots, 2 * tok_rows)),
                [payloads[c]] + riders,
                4 * slots * tok_rows * half,
            )
            sent.append(keep)
            sent.append(swap_ep(keep, 1))
            sent.append(swap_ep(pass_on, 2))
            sent.append(swap_ep(pass_on, 3))
            for _ in range(4):
                spans.append((at, slots))
                if riders:
                    rider_at.append(at + slots)
                at += size
        rows = jnp.concatenate(sent, axis=0)
        rows_other = swap_tp(rows)
        if rider_at:
            dense_parts = call(
                functools.partial(dense_part_kernel, planes, rider_at, rider_rows),
                (pltpu.VMEM((planes // 2, tok_rows, 4 * columns), bf16),) * 2,
                [rows, rows_other, *[payloads[c] for c in range(planes)]],
                32 * planes * tok_rows * shard.shape[0] * columns,
                [pltpu.VMEM((4 * shard.shape[0], 4 * columns), bf16)],
            )
        count = 4 * n * slots
        hidden = call(
            functools.partial(hidden_kernel, spans),
            shape(count, gate_weight.shape[1]),
            [rows, rows_other, gate_weight, up_weight],
            4 * count * model_width * gate_weight.shape[1],
        )
        hidden_other = swap_tp(hidden)
        parts = call(
            functools.partial(down_kernel, slots),
            (shape(slots, half),) * (4 * n),
            [hidden, hidden_other, down_weight],
            2 * count * down_weight.shape[0] * half,
        )
        for i, c in enumerate(group):
            kept, to_x, to_y, to_d = parts[4 * i : 4 * i + 4]
            mixed = call(
                combine_kernel,
                shape(tok_rows, half, bf16 if c else f32),
                [
                    kept,
                    swap_ep(to_x, 1),
                    swap_ep(to_y, 2),
                    swap_ep(to_d, 3),
                    spreads[c],
                    *relayed.pop(c, []),
                ],
                8 * slots * tok_rows * half,
            )
            if c == 0:
                results.append(mixed)
            elif c > 1 and c % 2 == 0:
                relayed[c + 1] = [swap_ep(mixed, 4)]
            else:
                results.append(swap_ep(mixed, 4 * c))

    near, away = dense_parts
    for bit in range(planes.bit_length() - 1):
        arrived = swap_active(away, 4 << bit, ep_count // 2)
        size = near.shape[0] // 2
        outs = (pltpu.VMEM((max(size, 1), tok_rows, 4 * columns), bf16 if size else f32),)
        near = call(add_kernel, outs * (2 if size else 1), [near, arrived], 10**6)
        near, away = near if size else (near[0], None)
    return call(
        finish_kernel,
        jax.ShapeDtypeStruct((tok_rows, half), bf16),
        [
            near,
            swap_tp(near),
            dense_down,
            branch_gate[None, :],
            *results,
        ],
        8 * tok_rows * columns * half,
    )


def chunk_groups(planes):
    return [[0, 1]] + [[c] for c in range(2, planes)]


def by_all_to_all(
    tokens,
    expert_ids,
    route_weights,
    norm_gain,
    gate_weight,
    up_weight,
    down_weight,
    dense_gate,
    dense_up,
    dense_down,
    branch_gate,
):
    tok_rows, model_width = tokens.shape
    top_count = expert_ids.shape[1]
    ep_count = lax.axis_size("ep")
    experts = ep_count // 2
    slot_count = 2 * top_count * tok_rows // experts
    values = tokens.astype(jnp.float32)
    inverse = lax.rsqrt(jnp.mean(values * values, axis=1, keepdims=True) + epsilon)
    normed = (values * inverse * norm_gain[None, :]).astype(jnp.bfloat16)
    dense_gate_act = jnp.dot(
        normed,
        lax.all_gather(dense_gate, "ep", axis=0, tiled=True),
        preferred_element_type=jnp.float32,
    )
    dense_up_act = jnp.dot(
        normed,
        lax.all_gather(dense_up, "ep", axis=0, tiled=True),
        preferred_element_type=jnp.float32,
    )
    dense_hidden = (jax.nn.silu(dense_gate_act) * dense_up_act).astype(jnp.bfloat16)
    dense_out = jnp.dot(dense_hidden, dense_down, preferred_element_type=jnp.float32)
    flat_ids = expert_ids.reshape(tok_rows * top_count)
    labels = lax.broadcasted_iota(jnp.int32, (1, experts), 1)
    onehot = (flat_ids[:, None] == labels).astype(jnp.int32)
    earlier = jnp.cumsum(onehot, axis=0) - onehot
    slot_index = jnp.sum(onehot * earlier, axis=1)
    row_code = (flat_ids * slot_count + slot_index).reshape(tok_rows, top_count)
    targets = lax.broadcasted_iota(jnp.int32, (experts * slot_count, 1, 1), 0)
    selector = jnp.any(row_code[None, :, :] == targets, axis=2).astype(jnp.bfloat16)
    buffer = jnp.dot(selector, normed, preferred_element_type=jnp.float32).astype(jnp.bfloat16)
    buffer = buffer.reshape(experts, slot_count, model_width)
    half = model_width // 2
    outgoing = lax.dynamic_slice_in_dim(
        jnp.repeat(buffer, 2, axis=0), lax.axis_index("tp") * half, half, 2
    )
    arrived = lax.all_gather(
        lax.all_to_all(outgoing, "ep", split_axis=0, concat_axis=0, tiled=True),
        "tp",
        axis=2,
        tiled=True,
    )
    in_rows = arrived.reshape(ep_count * slot_count, model_width)
    expert_gate = jnp.dot(in_rows, gate_weight, preferred_element_type=jnp.float32)
    expert_up = jnp.dot(in_rows, up_weight, preferred_element_type=jnp.float32)
    hidden = (jax.nn.silu(expert_gate) * expert_up).astype(jnp.bfloat16)
    down_total = jnp.dot(
        lax.all_gather(hidden, "tp", axis=1, tiled=True),
        down_weight,
        preferred_element_type=jnp.float32,
    )
    partial_value = down_total.astype(jnp.bfloat16).reshape(ep_count, slot_count, -1)
    returned_rows = lax.all_to_all(partial_value, "ep", split_axis=0, concat_axis=0, tiled=True)
    pair_sums = returned_rows.reshape(experts, 2, slot_count, -1).astype(jnp.float32)
    expert_out = (
        (pair_sums[:, 0] + pair_sums[:, 1]).astype(jnp.bfloat16).reshape(experts * slot_count, -1)
    )
    picked = (
        jnp.take(expert_out, row_code.reshape(-1), axis=0)
        .reshape(tok_rows, top_count, -1)
        .astype(jnp.float32)
    )
    routed = jnp.sum(route_weights[:, :, None] * picked, axis=1)
    mixed_out = routed + jax.nn.sigmoid(branch_gate)[None, :] * dense_out
    return mixed_out.astype(jnp.bfloat16)


def per_device(*args):
    tokens, expert_ids = args[:2]
    experts = lax.axis_size("ep") // 2
    slots = 2 * expert_ids.shape[1] * tokens.shape[0] // experts
    planes = experts // 2
    if planes > 1 and planes & (planes - 1) == 0 and 2 * slots >= tokens.shape[0]:
        return by_planes(*args)
    return by_all_to_all(*args)


def solution(mesh):
    in_specs = (
        P("ep", None),
        P("ep", None),
        P("ep", None),
        P(),
        P(None, ("ep", "tp")),
        P(None, ("ep", "tp")),
        P("ep", "tp"),
        P("ep", None),
        P("ep", None),
        P(None, "tp"),
        P("tp"),
    )
    return jax.shard_map(
        per_device, mesh=mesh, in_specs=in_specs, out_specs=P("ep", "tp"), check_vma=False
    )
```

```python
import functools

import jax
import jax.numpy as jnp
from jax import lax
from jax.experimental import pallas as pl
from jax.experimental.pallas import tpu as pltpu
from jax.sharding import PartitionSpec as P

epsilon = 1e-06
bf16 = jnp.bfloat16
f32 = jnp.float32
META_ROWS = 8


def swap_ep(value, mask):
    count = lax.axis_size("ep")
    return lax.ppermute(value, "ep", [(i, i ^ mask) for i in range(count)])


def swap_active(value, mask, per_half):
    count = lax.axis_size("ep")
    pairs = []
    for i in range(count):
        core = i // per_half
        pairs.append((2 * i + core, 2 * (i ^ mask) + core))
    return lax.ppermute(value, ("ep", "tp"), pairs)


def swap_tp(value):
    count = lax.axis_size("tp")
    return lax.ppermute(value, "tp", [(i, count - 1 - i) for i in range(count)])


def dot(a, b):
    return jnp.dot(a, b, preferred_element_type=f32)


def gated(gate, up):
    return (gate / (1.0 + jnp.exp(-gate)) * up).astype(bf16)


def call(kernel, outs, arrays, flops, scratch=()):
    moved = sum(a.size * a.dtype.itemsize for a in arrays)
    return pl.pallas_call(
        kernel,
        out_shape=outs,
        in_specs=[pl.BlockSpec(memory_space=pltpu.VMEM)] * len(arrays),
        out_specs=jax.tree.map(lambda _: pl.BlockSpec(memory_space=pltpu.VMEM), outs),
        cost_estimate=pl.CostEstimate(flops=flops, bytes_accessed=moved, transcendentals=0),
        compiler_params=pltpu.CompilerParams(vmem_limit_bytes=4 << 20),
        scratch_shapes=scratch,
    )(*[pltpu.with_memory_space_constraint(a, pltpu.VMEM) for a in arrays])


def shape(rows, columns, dtype=bf16):
    return pltpu.VMEM((rows, columns), dtype)


def both_halves(count):
    tp = lax.axis_index("tp")
    return [pl.ds(pl.multiple_of(i * count, count), count) for i in (tp, 1 - tp)]


def prepare_kernel(
    tokens_at,
    gain_at,
    ids_at,
    weights_at,
    gate_at,
    up_at,
    payload_ref,
    shard_ref,
    tokens_ref,
    gain_ref,
    ids_ref,
    weights_ref,
    normed_ref,
    sems,
):
    rows, width = tokens_ref.shape
    half = width // 2
    columns = shard_ref.shape[1] // 2
    mine = both_halves(columns)[0]
    copies = []
    for source, target in (
        (tokens_at, tokens_ref),
        (gain_at, gain_ref),
        (ids_at, ids_ref),
        (weights_at, weights_ref),
        (gate_at.at[:, mine], shard_ref.at[:, :columns]),
        (up_at.at[:, mine], shard_ref.at[:, columns:]),
    ):
        copies.append(pltpu.make_async_copy(source, target, sems.at[len(copies)]))
        copies[-1].start()
    for copy in copies[:4]:
        copy.wait()
    values = tokens_ref[...].astype(f32)
    inverse = lax.rsqrt(jnp.mean(values * values, axis=1, keepdims=True) + epsilon)
    normed_ref[...] = (values * inverse * gain_ref[...]).astype(bf16)
    payload_ref[:rows, :] = normed_ref[:, both_halves(half)[0]]
    payload_ref[rows:, :] = jnp.zeros((META_ROWS, half), bf16)
    weights = weights_ref[...]
    parts = [ids_ref[...].astype(f32)]
    for _ in range(3):
        parts.append(weights.astype(bf16).astype(f32))
        weights = weights - parts[-1]
    payload_ref[rows:, :rows] = jnp.concatenate(parts, axis=0).astype(bf16)
    for copy in copies[4:]:
        copy.wait()


def select_kernel(top, slots, payload_ref, *refs):
    rider_refs, (keep_ref, pass_ref, spread_ref) = refs[:-3], refs[-3:]
    tokens = payload_ref.shape[0] - META_ROWS
    before = (
        lax.broadcasted_iota(jnp.int32, (tokens, tokens), 0)
        < lax.broadcasted_iota(jnp.int32, (tokens, tokens), 1)
    ).astype(bf16)
    slot = lax.broadcasted_iota(jnp.int32, (slots, tokens), 0).astype(f32)
    meta = payload_ref[tokens:, :tokens].astype(f32)
    ids = meta[:top]
    weights = sum(meta[top * p : top * (p + 1)] for p in range(1, 4))
    for side, out_ref in enumerate((keep_ref, pass_ref)):
        match = ids == ((lax.axis_index("ep") // 2) ^ side).astype(f32)
        named = jnp.max(match.astype(f32), axis=0, keepdims=True)
        weight = jnp.sum(jnp.where(match, weights, 0.0), axis=0, keepdims=True)
        place = dot(jnp.broadcast_to(named, (META_ROWS, tokens)).astype(bf16), before)[:1]
        chosen = (place == slot) & (named > 0.0)
        out_ref[:slots, :] = dot(chosen.astype(bf16), payload_ref[:tokens, :]).astype(bf16)
        spread = jnp.where(chosen, weight, 0.0)
        high = spread.astype(bf16)
        low = (spread - high.astype(f32)).astype(bf16)
        here = slice(side * slots, (side + 1) * slots)
        spread_ref[here, :tokens] = high
        spread_ref[here, tokens:] = low
        for rider_ref in rider_refs:
            count, width = out_ref.shape[0] - slots, rider_ref.shape[1]
            for q in range(out_ref.shape[1] // width):
                out_ref[slots:, q * width : (q + 1) * width] = rider_ref[
                    q * count : (q + 1) * count, :
                ]


def hidden_kernel(spans, mine_ref, other_ref, gate_ref, up_ref, out_ref):
    mine, other = both_halves(mine_ref.shape[1])
    rows, rows_other = mine_ref[...], other_ref[...]
    gate = dot(rows, gate_ref[mine, :]) + dot(rows_other, gate_ref[other, :])
    up = dot(rows, up_ref[mine, :]) + dot(rows_other, up_ref[other, :])
    hidden = gated(gate, up)
    at = 0
    for start, count in spans:
        out_ref[at : at + count, :] = hidden[start : start + count]
        at += count


def down_kernel(plan, slots, *refs):
    out_refs = refs[len(refs) - len(plan) :]
    down_ref = refs[len(refs) - len(plan) - 1]
    hidden_refs = refs[: len(refs) - len(plan) - 1]
    mine, other = both_halves(hidden_refs[0].shape[1])
    totals = []
    for mine_ref, other_ref in zip(hidden_refs[::2], hidden_refs[1::2]):
        total = dot(mine_ref[...], down_ref[mine, :]) + dot(other_ref[...], down_ref[other, :])
        totals.append(total.astype(bf16))
    for out_ref, places in zip(out_refs, plan):
        for n, (g, at) in enumerate(places):
            out_ref[n * slots : (n + 1) * slots, :] = totals[g][at : at + slots]


def combine_kernel(n, kept0_ref, kept1_ref, passed0_ref, passed1_ref, spread_ref, *refs):
    out_ref = refs[-1]
    tokens = out_ref.shape[0]
    slots = spread_ref.shape[0] // 2
    rows = slice(n * slots, (n + 1) * slots)
    contract = (((0,), (0,)), ((), ()))
    total = None
    for side, (a_ref, b_ref) in enumerate(((kept0_ref, kept1_ref), (passed0_ref, passed1_ref))):
        both = (a_ref[rows, :].astype(f32) + b_ref[rows, :].astype(f32)).astype(bf16)
        at = side * slots
        for part in (slice(0, tokens), slice(tokens, 2 * tokens)):
            term = lax.dot_general(
                spread_ref[at : at + slots, part], both, contract, preferred_element_type=f32
            )
            total = term if total is None else total + term
    for ref in refs[:-1]:
        total = total + ref[...].astype(f32)
    out_ref[...] = total.astype(out_ref.dtype)


def dense_part_kernel(planes, rider_at, rider_rows, rows_ref, other_ref, *refs):
    payload_refs, out_refs, weights_ref = refs[:planes], refs[planes:-1], refs[-1]
    tokens = payload_refs[0].shape[0] - META_ROWS
    block = weights_ref.shape[0] // 4
    width = weights_ref.shape[1] // 2
    ep = lax.axis_index("ep")
    for i in range(4):
        first = rider_at[i]
        for side, source_ref in enumerate((rows_ref, other_ref)):
            for q in range(block // rider_rows):
                at = pl.multiple_of(((ep ^ i) % 4) * block + q * rider_rows, rider_rows)
                weights_ref[pl.ds(at, rider_rows), side * width : (side + 1) * width] = source_ref[
                    first : first + rider_rows, q * width : (q + 1) * width
                ]
    half_planes = planes // 2
    active = (ep // 4 // half_planes == lax.axis_index("tp")).astype(f32)
    start = pl.multiple_of((ep // 4) % half_planes * 4 * block, 4 * block)
    for n, payload_ref in enumerate(payload_refs):
        part = dot(payload_ref[:tokens, pl.ds(start, 4 * block)], weights_ref[...])
        part = (part * active).astype(bf16)
        out_refs[n % 2][n // 2] = part


def add_kernel(a_ref, b_ref, *out_refs):
    for n in range(a_ref.shape[0]):
        out_ref = out_refs[n % len(out_refs)]
        total = a_ref[n].astype(f32) + b_ref[n].astype(f32)
        out_ref[n // len(out_refs)] = total.astype(out_ref.dtype)


def dense_out_kernel(mine_ref, other_ref, down_ref, branch_ref, out_ref):
    mine, other = mine_ref[0], other_ref[0]
    width = mine.shape[1] // 2
    count = width // 2
    dense = None
    for at, sums in zip(
        both_halves(count), (mine[:, :width] + other[:, width:], mine[:, width:] + other[:, :width])
    ):
        term = dot(gated(sums[:, :count], sums[:, count:]), down_ref[at, :])
        dense = term if dense is None else dense + term
    out_ref[...] = jax.nn.sigmoid(branch_ref[...]) * dense


def finish_kernel(*refs):
    total = refs[0][...].astype(f32)
    for ref in refs[1:-1]:
        total = total + ref[...].astype(f32)
    refs[-1][...] = total.astype(bf16)


def by_planes(
    tokens,
    expert_ids,
    route_weights,
    norm_gain,
    gate_weight,
    up_weight,
    down_weight,
    dense_gate,
    dense_up,
    dense_down,
    branch_gate,
):
    tok_rows, model_width = tokens.shape
    top = expert_ids.shape[1]
    ep_count = lax.axis_size("ep")
    experts = ep_count // 2
    slots = 2 * top * tok_rows // experts
    planes = ep_count // 4
    half = model_width // 2

    columns = dense_gate.shape[1] // 2
    rows = dense_gate.shape[0]
    inputs = [tokens, norm_gain[None, :], expert_ids.T, route_weights.T, dense_gate, dense_up]
    payload, shard = pl.pallas_call(
        prepare_kernel,
        out_shape=(shape(tok_rows + META_ROWS, half), shape(rows, 2 * columns)),
        in_specs=[pl.BlockSpec(memory_space=pltpu.HBM)] * len(inputs),
        out_specs=[pl.BlockSpec(memory_space=pltpu.VMEM)] * 2,
        scratch_shapes=[pltpu.VMEM(a.shape, a.dtype) for a in inputs[:4]]
        + [pltpu.VMEM(tokens.shape, bf16), pltpu.SemaphoreType.DMA((len(inputs),))],
        compiler_params=pltpu.CompilerParams(vmem_limit_bytes=4 << 20),
        name="prepare",
    )(*[pltpu.with_memory_space_constraint(a, pltpu.HBM) for a in inputs])
    payloads = {0: payload}
    for c in range(1, planes):
        low = c & -c
        payloads[c] = swap_ep(payloads[c ^ low], 4 * low)

    rider_rows = shard.size // half

    results, relayed, dense_parts, spreads, hiddens = [], {}, None, {}, {}
    for group in chunk_groups(planes):
        n, g = len(group), group[0]
        sent, spans, rider_at, at = [], [], [], 0
        for c in group:
            riders = [] if c else [shard]
            size = slots + len(riders) * rider_rows
            keep, pass_on, spreads[c] = call(
                functools.partial(select_kernel, top, slots),
                (shape(size, half), shape(size, half), shape(2 * slots, 2 * tok_rows)),
                [payloads[c]] + riders,
                4 * slots * tok_rows * half,
            )
            sent.append(keep)
            sent.append(swap_ep(keep, 1))
            sent.append(swap_ep(pass_on, 2))
            sent.append(swap_ep(pass_on, 3))
            for _ in range(4):
                spans.append((at, slots))
                if riders:
                    rider_at.append(at + slots)
                at += size
        rows = jnp.concatenate(sent, axis=0)
        rows_other = swap_tp(rows)
        if rider_at:
            dense_parts = call(
                functools.partial(dense_part_kernel, planes, rider_at, rider_rows),
                (pltpu.VMEM((planes // 2, tok_rows, 4 * columns), bf16),) * 2,
                [rows, rows_other, *[payloads[c] for c in range(planes)]],
                32 * planes * tok_rows * shard.shape[0] * columns,
                [pltpu.VMEM((4 * shard.shape[0], 4 * columns), bf16)],
            )
        count = 4 * n * slots
        hidden = call(
            functools.partial(hidden_kernel, spans),
            shape(count, gate_weight.shape[1]),
            [rows, rows_other, gate_weight, up_weight],
            4 * count * model_width * gate_weight.shape[1],
        )
        hiddens[g] = [hidden, swap_tp(hidden)]

    for groups, returns in return_groups(planes):
        where = {c: (i, 4 * slots * n) for i, group in enumerate(groups) for n, c in enumerate(group)}
        plan = []
        for back in returns:
            for piece in range(4):
                plan.append([(where[c][0], where[c][1] + piece * slots) for c in back])
        count = 4 * slots * len(where)
        parts = call(
            functools.partial(down_kernel, plan, slots),
            tuple(shape(len(places) * slots, half) for places in plan),
            [value for group in groups for value in hiddens[group[0]]] + [down_weight],
            2 * count * down_weight.shape[0] * half,
        )
        for i, back in enumerate(returns):
            kept, to_x, to_y, to_d = parts[4 * i : 4 * i + 4]
            pieces = [kept, swap_ep(to_x, 1), swap_ep(to_y, 2), swap_ep(to_d, 3)]
            for n, c in enumerate(back):
                mixed = call(
                    functools.partial(combine_kernel, n),
                    shape(tok_rows, half, bf16 if c else f32),
                    [*pieces, spreads[c], *relayed.pop(c, [])],
                    8 * slots * tok_rows * half,
                )
                if c == 0:
                    results.append(mixed)
                elif c > 1 and c % 2 == 0:
                    relayed[c + 1] = [swap_ep(mixed, 4)]
                else:
                    results.append(swap_ep(mixed, 4 * c))

    near, away = dense_parts
    for bit in range(planes.bit_length() - 1):
        arrived = swap_active(away, 4 << bit, ep_count // 2) if bit else swap_ep(away, 4)
        size = near.shape[0] // 2
        outs = (pltpu.VMEM((max(size, 1), tok_rows, 4 * columns), bf16 if size else f32),)
        near = call(add_kernel, outs * (2 if size else 1), [near, arrived], 10**6)
        near, away = near if size else (near[0], None)
    dense_out = call(
        dense_out_kernel,
        shape(tok_rows, half, f32),
        [near, swap_tp(near), dense_down, branch_gate[None, :]],
        8 * tok_rows * columns * half,
    )
    return call(
        finish_kernel, jax.ShapeDtypeStruct((tok_rows, half), bf16), [dense_out, *results], 10**6
    )


def chunk_groups(planes):
    return [[0, 1]] + [[c] for c in range(2, planes)]


def return_groups(planes):
    return [([group], [[c] for c in group]) for group in chunk_groups(planes)]


def by_all_to_all(
    tokens,
    expert_ids,
    route_weights,
    norm_gain,
    gate_weight,
    up_weight,
    down_weight,
    dense_gate,
    dense_up,
    dense_down,
    branch_gate,
):
    tok_rows, model_width = tokens.shape
    top_count = expert_ids.shape[1]
    ep_count = lax.axis_size("ep")
    experts = ep_count // 2
    slot_count = 2 * top_count * tok_rows // experts
    values = tokens.astype(jnp.float32)
    inverse = lax.rsqrt(jnp.mean(values * values, axis=1, keepdims=True) + epsilon)
    normed = (values * inverse * norm_gain[None, :]).astype(jnp.bfloat16)
    dense_gate_act = jnp.dot(
        normed,
        lax.all_gather(dense_gate, "ep", axis=0, tiled=True),
        preferred_element_type=jnp.float32,
    )
    dense_up_act = jnp.dot(
        normed,
        lax.all_gather(dense_up, "ep", axis=0, tiled=True),
        preferred_element_type=jnp.float32,
    )
    dense_hidden = (jax.nn.silu(dense_gate_act) * dense_up_act).astype(jnp.bfloat16)
    dense_out = jnp.dot(dense_hidden, dense_down, preferred_element_type=jnp.float32)
    flat_ids = expert_ids.reshape(tok_rows * top_count)
    labels = lax.broadcasted_iota(jnp.int32, (1, experts), 1)
    onehot = (flat_ids[:, None] == labels).astype(jnp.int32)
    earlier = jnp.cumsum(onehot, axis=0) - onehot
    slot_index = jnp.sum(onehot * earlier, axis=1)
    row_code = (flat_ids * slot_count + slot_index).reshape(tok_rows, top_count)
    targets = lax.broadcasted_iota(jnp.int32, (experts * slot_count, 1, 1), 0)
    selector = jnp.any(row_code[None, :, :] == targets, axis=2).astype(jnp.bfloat16)
    buffer = jnp.dot(selector, normed, preferred_element_type=jnp.float32).astype(jnp.bfloat16)
    buffer = buffer.reshape(experts, slot_count, model_width)
    half = model_width // 2
    outgoing = lax.dynamic_slice_in_dim(
        jnp.repeat(buffer, 2, axis=0), lax.axis_index("tp") * half, half, 2
    )
    arrived = lax.all_gather(
        lax.all_to_all(outgoing, "ep", split_axis=0, concat_axis=0, tiled=True),
        "tp",
        axis=2,
        tiled=True,
    )
    in_rows = arrived.reshape(ep_count * slot_count, model_width)
    expert_gate = jnp.dot(in_rows, gate_weight, preferred_element_type=jnp.float32)
    expert_up = jnp.dot(in_rows, up_weight, preferred_element_type=jnp.float32)
    hidden = (jax.nn.silu(expert_gate) * expert_up).astype(jnp.bfloat16)
    down_total = jnp.dot(
        lax.all_gather(hidden, "tp", axis=1, tiled=True),
        down_weight,
        preferred_element_type=jnp.float32,
    )
    partial_value = down_total.astype(jnp.bfloat16).reshape(ep_count, slot_count, -1)
    returned_rows = lax.all_to_all(partial_value, "ep", split_axis=0, concat_axis=0, tiled=True)
    pair_sums = returned_rows.reshape(experts, 2, slot_count, -1).astype(jnp.float32)
    expert_out = (
        (pair_sums[:, 0] + pair_sums[:, 1]).astype(jnp.bfloat16).reshape(experts * slot_count, -1)
    )
    picked = (
        jnp.take(expert_out, row_code.reshape(-1), axis=0)
        .reshape(tok_rows, top_count, -1)
        .astype(jnp.float32)
    )
    routed = jnp.sum(route_weights[:, :, None] * picked, axis=1)
    mixed_out = routed + jax.nn.sigmoid(branch_gate)[None, :] * dense_out
    return mixed_out.astype(jnp.bfloat16)


def per_device(*args):
    tokens, expert_ids = args[:2]
    experts = lax.axis_size("ep") // 2
    slots = 2 * expert_ids.shape[1] * tokens.shape[0] // experts
    planes = experts // 2
    if planes > 1 and planes & (planes - 1) == 0 and 2 * slots >= tokens.shape[0]:
        return by_planes(*args)
    return by_all_to_all(*args)


def solution(mesh):
    in_specs = (
        P("ep", None),
        P("ep", None),
        P("ep", None),
        P(),
        P(None, ("ep", "tp")),
        P(None, ("ep", "tp")),
        P("ep", "tp"),
        P("ep", None),
        P("ep", None),
        P(None, "tp"),
        P("tp"),
    )
    return jax.shard_map(
        per_device, mesh=mesh, in_specs=in_specs, out_specs=P("ep", "tp"), check_vma=False
    )
```

```python
import functools

import jax
import jax.numpy as jnp
from jax import lax
from jax.experimental import pallas as pl
from jax.experimental.pallas import tpu as pltpu
from jax.sharding import PartitionSpec as P

epsilon = 1e-06
bf16 = jnp.bfloat16
f32 = jnp.float32
META_ROWS = 8


def swap_ep(value, mask):
    count = lax.axis_size("ep")
    return lax.ppermute(value, "ep", [(i, i ^ mask) for i in range(count)])


def swap_tp(value):
    count = lax.axis_size("tp")
    return lax.ppermute(value, "tp", [(i, count - 1 - i) for i in range(count)])


def dot(a, b):
    return jnp.dot(a, b, preferred_element_type=f32)


def gated(gate, up):
    return (gate / (1.0 + jnp.exp(-gate)) * up).astype(bf16)


def call(kernel, outs, arrays, flops, scratch=()):
    moved = sum(a.size * a.dtype.itemsize for a in arrays)
    return pl.pallas_call(
        kernel,
        out_shape=outs,
        in_specs=[pl.BlockSpec(memory_space=pltpu.VMEM)] * len(arrays),
        out_specs=jax.tree.map(lambda _: pl.BlockSpec(memory_space=pltpu.VMEM), outs),
        cost_estimate=pl.CostEstimate(flops=flops, bytes_accessed=moved, transcendentals=0),
        compiler_params=pltpu.CompilerParams(vmem_limit_bytes=4 << 20),
        scratch_shapes=scratch,
    )(*[pltpu.with_memory_space_constraint(a, pltpu.VMEM) for a in arrays])


def shape(rows, columns, dtype=bf16):
    return pltpu.VMEM((rows, columns), dtype)


def both_halves(count):
    tp = lax.axis_index("tp")
    return [pl.ds(pl.multiple_of(i * count, count), count) for i in (tp, 1 - tp)]


def prepare_kernel(
    tokens_at,
    gain_at,
    ids_at,
    weights_at,
    gate_at,
    up_at,
    payload_ref,
    shard_ref,
    tokens_ref,
    gain_ref,
    ids_ref,
    weights_ref,
    normed_ref,
    sems,
):
    rows, width = tokens_ref.shape
    half = width // 2
    columns = shard_ref.shape[1] // 2
    mine = both_halves(columns)[0]
    copies = []
    for source, target in (
        (tokens_at, tokens_ref),
        (gain_at, gain_ref),
        (ids_at, ids_ref),
        (weights_at, weights_ref),
        (gate_at.at[:, mine], shard_ref.at[:, :columns]),
        (up_at.at[:, mine], shard_ref.at[:, columns:]),
    ):
        copies.append(pltpu.make_async_copy(source, target, sems.at[len(copies)]))
        copies[-1].start()
    for copy in copies[:4]:
        copy.wait()
    values = tokens_ref[...].astype(f32)
    inverse = lax.rsqrt(jnp.mean(values * values, axis=1, keepdims=True) + epsilon)
    normed_ref[...] = (values * inverse * gain_ref[...]).astype(bf16)
    payload_ref[:rows, :] = normed_ref[:, both_halves(half)[0]]
    payload_ref[rows:, :] = jnp.zeros((META_ROWS, half), bf16)
    weights = weights_ref[...]
    parts = [ids_ref[...].astype(f32)]
    for _ in range(3):
        parts.append(weights.astype(bf16).astype(f32))
        weights = weights - parts[-1]
    payload_ref[rows:, :rows] = jnp.concatenate(parts, axis=0).astype(bf16)
    for copy in copies[4:]:
        copy.wait()


def select_kernel(top, slots, payload_ref, *refs):
    rider_refs, (keep_ref, pass_ref, spread_ref) = refs[:-3], refs[-3:]
    tokens = payload_ref.shape[0] - META_ROWS
    before = (
        lax.broadcasted_iota(jnp.int32, (tokens, tokens), 0)
        < lax.broadcasted_iota(jnp.int32, (tokens, tokens), 1)
    ).astype(bf16)
    slot = lax.broadcasted_iota(jnp.int32, (slots, tokens), 0).astype(f32)
    meta = payload_ref[tokens:, :tokens].astype(f32)
    ids = meta[:top]
    weights = sum(meta[top * p : top * (p + 1)] for p in range(1, 4))
    for side, out_ref in enumerate((keep_ref, pass_ref)):
        match = ids == ((lax.axis_index("ep") // 2) ^ side).astype(f32)
        named = jnp.max(match.astype(f32), axis=0, keepdims=True)
        weight = jnp.sum(jnp.where(match, weights, 0.0), axis=0, keepdims=True)
        place = dot(jnp.broadcast_to(named, (META_ROWS, tokens)).astype(bf16), before)[:1]
        chosen = (place == slot) & (named > 0.0)
        out_ref[:slots, :] = dot(chosen.astype(bf16), payload_ref[:tokens, :]).astype(bf16)
        spread = jnp.where(chosen, weight, 0.0)
        high = spread.astype(bf16)
        low = (spread - high.astype(f32)).astype(bf16)
        here = slice(side * slots, (side + 1) * slots)
        spread_ref[here, :tokens] = high
        spread_ref[here, tokens:] = low
        for rider_ref in rider_refs:
            count, width = out_ref.shape[0] - slots, rider_ref.shape[1]
            for q in range(out_ref.shape[1] // width):
                out_ref[slots:, q * width : (q + 1) * width] = rider_ref[
                    q * count : (q + 1) * count, :
                ]


def hidden_kernel(spans, mine_ref, other_ref, gate_ref, up_ref, out_ref):
    mine, other = both_halves(mine_ref.shape[1])
    rows, rows_other = mine_ref[...], other_ref[...]
    gate = dot(rows, gate_ref[mine, :]) + dot(rows_other, gate_ref[other, :])
    up = dot(rows, up_ref[mine, :]) + dot(rows_other, up_ref[other, :])
    hidden = gated(gate, up)
    at = 0
    for start, count in spans:
        out_ref[at : at + count, :] = hidden[start : start + count]
        at += count


def down_kernel(plan, slots, *refs):
    out_refs = refs[len(refs) - len(plan) :]
    down_ref = refs[len(refs) - len(plan) - 1]
    hidden_refs = refs[: len(refs) - len(plan) - 1]
    mine, other = both_halves(hidden_refs[0].shape[1])
    totals = []
    for mine_ref, other_ref in zip(hidden_refs[::2], hidden_refs[1::2]):
        total = dot(mine_ref[...], down_ref[mine, :]) + dot(other_ref[...], down_ref[other, :])
        totals.append(total.astype(bf16))
    for out_ref, places in zip(out_refs, plan):
        for n, (g, at) in enumerate(places):
            out_ref[n * slots : (n + 1) * slots, :] = totals[g][at : at + slots]


def combine_kernel(n, kept0_ref, kept1_ref, passed0_ref, passed1_ref, spread_ref, *refs):
    out_ref = refs[-1]
    tokens = out_ref.shape[0]
    slots = spread_ref.shape[0] // 2
    rows = slice(n * slots, (n + 1) * slots)
    contract = (((0,), (0,)), ((), ()))
    total = None
    for side, (a_ref, b_ref) in enumerate(((kept0_ref, kept1_ref), (passed0_ref, passed1_ref))):
        both = (a_ref[rows, :].astype(f32) + b_ref[rows, :].astype(f32)).astype(bf16)
        at = side * slots
        for part in (slice(0, tokens), slice(tokens, 2 * tokens)):
            term = lax.dot_general(
                spread_ref[at : at + slots, part], both, contract, preferred_element_type=f32
            )
            total = term if total is None else total + term
    for ref in refs[:-1]:
        total = total + ref[...].astype(f32)
    out_ref[...] = total.astype(out_ref.dtype)


def dense_part_kernel(planes, rider_at, rider_rows, rows_ref, other_ref, *refs):
    payload_refs, out_refs, weights_ref = refs[:planes], refs[planes:-1], refs[-1]
    tokens = payload_refs[0].shape[0] - META_ROWS
    block = weights_ref.shape[0] // 4
    width = weights_ref.shape[1] // 2
    ep = lax.axis_index("ep")
    for i in range(4):
        first = rider_at[i]
        for side, source_ref in enumerate((rows_ref, other_ref)):
            for q in range(block // rider_rows):
                at = pl.multiple_of(((ep ^ i) % 4) * block + q * rider_rows, rider_rows)
                weights_ref[pl.ds(at, rider_rows), side * width : (side + 1) * width] = source_ref[
                    first : first + rider_rows, q * width : (q + 1) * width
                ]
    half_planes = planes // 2
    active = (ep // 4 // half_planes == lax.axis_index("tp")).astype(f32)
    start = pl.multiple_of((ep // 4) % half_planes * 4 * block, 4 * block)
    for n, payload_ref in enumerate(payload_refs):
        part = dot(payload_ref[:tokens, pl.ds(start, 4 * block)], weights_ref[...])
        part = (part * active).astype(bf16)
        out_refs[n % 2][n // 2] = part


def add_kernel(a_ref, b_ref, *out_refs):
    for n in range(a_ref.shape[0]):
        out_ref = out_refs[n % len(out_refs)]
        total = a_ref[n].astype(f32) + b_ref[n].astype(f32)
        out_ref[n // len(out_refs)] = total.astype(out_ref.dtype)


def dense_out_kernel(mine_ref, other_ref, down_ref, branch_ref, out_ref):
    mine, other = mine_ref[0], other_ref[0]
    width = mine.shape[1] // 2
    count = width // 2
    dense = None
    for at, sums in zip(
        both_halves(count), (mine[:, :width] + other[:, width:], mine[:, width:] + other[:, :width])
    ):
        term = dot(gated(sums[:, :count], sums[:, count:]), down_ref[at, :])
        dense = term if dense is None else dense + term
    out_ref[...] = jax.nn.sigmoid(branch_ref[...]) * dense


def finish_kernel(*refs):
    total = refs[0][...].astype(f32)
    for ref in refs[1:-1]:
        total = total + ref[...].astype(f32)
    refs[-1][...] = total.astype(bf16)


def by_planes(
    tokens,
    expert_ids,
    route_weights,
    norm_gain,
    gate_weight,
    up_weight,
    down_weight,
    dense_gate,
    dense_up,
    dense_down,
    branch_gate,
):
    tok_rows, model_width = tokens.shape
    top = expert_ids.shape[1]
    ep_count = lax.axis_size("ep")
    experts = ep_count // 2
    slots = 2 * top * tok_rows // experts
    planes = ep_count // 4
    half = model_width // 2

    columns = dense_gate.shape[1] // 2
    rows = dense_gate.shape[0]
    inputs = [tokens, norm_gain[None, :], expert_ids.T, route_weights.T, dense_gate, dense_up]
    payload, shard = pl.pallas_call(
        prepare_kernel,
        out_shape=(shape(tok_rows + META_ROWS, half), shape(rows, 2 * columns)),
        in_specs=[pl.BlockSpec(memory_space=pltpu.HBM)] * len(inputs),
        out_specs=[pl.BlockSpec(memory_space=pltpu.VMEM)] * 2,
        scratch_shapes=[pltpu.VMEM(a.shape, a.dtype) for a in inputs[:4]]
        + [pltpu.VMEM(tokens.shape, bf16), pltpu.SemaphoreType.DMA((len(inputs),))],
        compiler_params=pltpu.CompilerParams(vmem_limit_bytes=4 << 20),
        name="prepare",
    )(*[pltpu.with_memory_space_constraint(a, pltpu.HBM) for a in inputs])
    payloads = {0: payload}
    for c in range(1, planes):
        low = c & -c
        payloads[c] = swap_ep(payloads[c ^ low], 4 * low)

    rider_rows = shard.size // half

    results, relayed, dense_parts, spreads, hiddens = [], {}, None, {}, {}
    for group in chunk_groups(planes):
        n, g = len(group), group[0]
        sent, spans, rider_at, at = [], [], [], 0
        for c in group:
            riders = [] if c else [shard]
            size = slots + len(riders) * rider_rows
            keep, pass_on, spreads[c] = call(
                functools.partial(select_kernel, top, slots),
                (shape(size, half), shape(size, half), shape(2 * slots, 2 * tok_rows)),
                [payloads[c]] + riders,
                4 * slots * tok_rows * half,
            )
            sent.append(keep)
            sent.append(swap_ep(keep, 1))
            sent.append(swap_ep(pass_on, 2))
            sent.append(swap_ep(pass_on, 3))
            for _ in range(4):
                spans.append((at, slots))
                if riders:
                    rider_at.append(at + slots)
                at += size
        rows = jnp.concatenate(sent, axis=0)
        rows_other = swap_tp(rows)
        if rider_at:
            dense_parts = call(
                functools.partial(dense_part_kernel, planes, rider_at, rider_rows),
                (pltpu.VMEM((planes // 2, tok_rows, 4 * columns), bf16),) * 2,
                [rows, rows_other, *[payloads[c] for c in range(planes)]],
                32 * planes * tok_rows * shard.shape[0] * columns,
                [pltpu.VMEM((4 * shard.shape[0], 4 * columns), bf16)],
            )
        count = 4 * n * slots
        hidden = call(
            functools.partial(hidden_kernel, spans),
            shape(count, gate_weight.shape[1]),
            [rows, rows_other, gate_weight, up_weight],
            4 * count * model_width * gate_weight.shape[1],
        )
        hiddens[g] = [hidden, swap_tp(hidden)]

    for groups, returns in return_groups(planes):
        where = {c: (i, 4 * slots * n) for i, group in enumerate(groups) for n, c in enumerate(group)}
        plan = []
        for back in returns:
            for piece in range(4):
                plan.append([(where[c][0], where[c][1] + piece * slots) for c in back])
        count = 4 * slots * len(where)
        parts = call(
            functools.partial(down_kernel, plan, slots),
            tuple(shape(len(places) * slots, half) for places in plan),
            [value for group in groups for value in hiddens[group[0]]] + [down_weight],
            2 * count * down_weight.shape[0] * half,
        )
        for i, back in enumerate(returns):
            kept, to_x, to_y, to_d = parts[4 * i : 4 * i + 4]
            pieces = [kept, swap_ep(to_x, 1), swap_ep(to_y, 2), swap_ep(to_d, 3)]
            for n, c in enumerate(back):
                mixed = call(
                    functools.partial(combine_kernel, n),
                    shape(tok_rows, half, bf16 if c else f32),
                    [*pieces, spreads[c], *relayed.pop(c, [])],
                    8 * slots * tok_rows * half,
                )
                if c == 0:
                    results.append(mixed)
                elif c > 1 and c % 2 == 0:
                    relayed[c + 1] = [swap_ep(mixed, 4)]
                else:
                    results.append(swap_ep(mixed, 4 * c))

    near, away = dense_parts
    for bit in range(planes.bit_length() - 1):
        arrived = swap_ep(away, 4 << bit)
        size = near.shape[0] // 2
        outs = (pltpu.VMEM((max(size, 1), tok_rows, 4 * columns), bf16 if size else f32),)
        near = call(add_kernel, outs * (2 if size else 1), [near, arrived], 10**6)
        near, away = near if size else (near[0], None)
    dense_out = call(
        dense_out_kernel,
        shape(tok_rows, half, f32),
        [near, swap_tp(near), dense_down, branch_gate[None, :]],
        8 * tok_rows * columns * half,
    )
    return call(
        finish_kernel, jax.ShapeDtypeStruct((tok_rows, half), bf16), [dense_out, *results], 10**6
    )


def chunk_groups(planes):
    return [[0, 1]] + [[c] for c in range(2, planes)]


def return_groups(planes):
    return [([group], [[c] for c in group]) for group in chunk_groups(planes)]


def by_all_to_all(
    tokens,
    expert_ids,
    route_weights,
    norm_gain,
    gate_weight,
    up_weight,
    down_weight,
    dense_gate,
    dense_up,
    dense_down,
    branch_gate,
):
    tok_rows, model_width = tokens.shape
    top_count = expert_ids.shape[1]
    ep_count = lax.axis_size("ep")
    experts = ep_count // 2
    slot_count = 2 * top_count * tok_rows // experts
    values = tokens.astype(jnp.float32)
    inverse = lax.rsqrt(jnp.mean(values * values, axis=1, keepdims=True) + epsilon)
    normed = (values * inverse * norm_gain[None, :]).astype(jnp.bfloat16)
    dense_gate_act = jnp.dot(
        normed,
        lax.all_gather(dense_gate, "ep", axis=0, tiled=True),
        preferred_element_type=jnp.float32,
    )
    dense_up_act = jnp.dot(
        normed,
        lax.all_gather(dense_up, "ep", axis=0, tiled=True),
        preferred_element_type=jnp.float32,
    )
    dense_hidden = (jax.nn.silu(dense_gate_act) * dense_up_act).astype(jnp.bfloat16)
    dense_out = jnp.dot(dense_hidden, dense_down, preferred_element_type=jnp.float32)
    flat_ids = expert_ids.reshape(tok_rows * top_count)
    labels = lax.broadcasted_iota(jnp.int32, (1, experts), 1)
    onehot = (flat_ids[:, None] == labels).astype(jnp.int32)
    earlier = jnp.cumsum(onehot, axis=0) - onehot
    slot_index = jnp.sum(onehot * earlier, axis=1)
    row_code = (flat_ids * slot_count + slot_index).reshape(tok_rows, top_count)
    targets = lax.broadcasted_iota(jnp.int32, (experts * slot_count, 1, 1), 0)
    selector = jnp.any(row_code[None, :, :] == targets, axis=2).astype(jnp.bfloat16)
    buffer = jnp.dot(selector, normed, preferred_element_type=jnp.float32).astype(jnp.bfloat16)
    buffer = buffer.reshape(experts, slot_count, model_width)
    half = model_width // 2
    outgoing = lax.dynamic_slice_in_dim(
        jnp.repeat(buffer, 2, axis=0), lax.axis_index("tp") * half, half, 2
    )
    arrived = lax.all_gather(
        lax.all_to_all(outgoing, "ep", split_axis=0, concat_axis=0, tiled=True),
        "tp",
        axis=2,
        tiled=True,
    )
    in_rows = arrived.reshape(ep_count * slot_count, model_width)
    expert_gate = jnp.dot(in_rows, gate_weight, preferred_element_type=jnp.float32)
    expert_up = jnp.dot(in_rows, up_weight, preferred_element_type=jnp.float32)
    hidden = (jax.nn.silu(expert_gate) * expert_up).astype(jnp.bfloat16)
    down_total = jnp.dot(
        lax.all_gather(hidden, "tp", axis=1, tiled=True),
        down_weight,
        preferred_element_type=jnp.float32,
    )
    partial_value = down_total.astype(jnp.bfloat16).reshape(ep_count, slot_count, -1)
    returned_rows = lax.all_to_all(partial_value, "ep", split_axis=0, concat_axis=0, tiled=True)
    pair_sums = returned_rows.reshape(experts, 2, slot_count, -1).astype(jnp.float32)
    expert_out = (
        (pair_sums[:, 0] + pair_sums[:, 1]).astype(jnp.bfloat16).reshape(experts * slot_count, -1)
    )
    picked = (
        jnp.take(expert_out, row_code.reshape(-1), axis=0)
        .reshape(tok_rows, top_count, -1)
        .astype(jnp.float32)
    )
    routed = jnp.sum(route_weights[:, :, None] * picked, axis=1)
    mixed_out = routed + jax.nn.sigmoid(branch_gate)[None, :] * dense_out
    return mixed_out.astype(jnp.bfloat16)


def per_device(*args):
    tokens, expert_ids = args[:2]
    experts = lax.axis_size("ep") // 2
    slots = 2 * expert_ids.shape[1] * tokens.shape[0] // experts
    planes = experts // 2
    if planes > 1 and planes & (planes - 1) == 0 and 2 * slots >= tokens.shape[0]:
        return by_planes(*args)
    return by_all_to_all(*args)


def solution(mesh):
    in_specs = (
        P("ep", None),
        P("ep", None),
        P("ep", None),
        P(),
        P(None, ("ep", "tp")),
        P(None, ("ep", "tp")),
        P("ep", "tp"),
        P("ep", None),
        P("ep", None),
        P(None, "tp"),
        P("tp"),
    )
    return jax.shard_map(
        per_device, mesh=mesh, in_specs=in_specs, out_specs=P("ep", "tp"), check_vma=False
    )
```
